128 devices in a mesh: fs: 32 (over z, y, core), tp: 4 (over x).
Axes of the slice: x: 4, y: 4, z: 4, core: 2. Of those that a mesh axis runs over, the one named last changes fastest.
Arguments:
- normed_input: bfloat16 [147456, 2048], P('fs'), may hold values from -12 to 12
- query_latent_cotangent: bfloat16 [147456, 768], P('fs', 'tp'), may hold values from -0.015625 to 0.015625
- key_value_latent_cotangent: bfloat16 [147456, 512], P('fs', 'tp'), may hold values from -0.015625 to 0.015625
- row_factor: bfloat16 [2048, 256], P('fs'), may hold values from -0.25 to 0.25
- query_down_weight: float32 [2048, 768], P('fs', 'tp'), may hold values from -6 to 6
- key_value_down_weight: float32 [2048, 512], P('fs', 'tp'), may hold values from -6 to 6
- query_first_moment: float32 [256, 768], P('fs', 'tp'), may hold values from -6 to 6
- key_value_first_moment: float32 [256, 512], P('fs', 'tp'), may hold values from -6 to 6
- query_second: float32 [256, 768], P('fs', 'tp'), may hold values from 0.5 to 2000
- latent_second: float32 [256, 512], P('fs', 'tp'), may hold values from 0.5 to 2000
Outputs:
- query_new: float32 [2048, 768], P('fs', 'tp')
- latent_new: float32 [2048, 512], P('fs', 'tp')
- query_step: float32 [2048, 768], P('fs', 'tp')
- latent_step: float32 [2048, 512], P('fs', 'tp')
- query_copy: bfloat16 [2048, 768], P(None, 'tp')
- latent_copy: bfloat16 [2048, 512], P(None, 'tp')
- query_first_new: float32 [256, 768], P('fs', 'tp')
- latent_first_new: float32 [256, 512], P('fs', 'tp')
- query_second_new: float32 [256, 768], P('fs', 'tp')
- latent_second_new: float32 [256, 512], P('fs', 'tp')
The draws below stay inside these ranges and needn't reach their ends.
All inputs are finite; a program needn't handle non-finite values.
Results may differ from the reference program's by a relative error of at most 0.006.
Values may be sent and summed in bfloat16 or wider, within the bound.
A program may use at most 64 MiB of HBM per device.

```python
import jax
import jax.numpy as jnp
from jax import lax

MODEL_WIDTH = 2048
QUERY_LATENT = 768
KEY_VALUE_LATENT = 512
PROJECTION_RANK = 256
TOKEN_TOTAL = 147456


def second_moment_estimate(key, rows, cols):
    key_two = jax.random.fold_in(key, 1)
    row_index = jnp.arange(rows, dtype=jnp.float32) / max(rows - 1, 1)
    col_index = jnp.arange(cols, dtype=jnp.float32) / max(cols - 1, 1)
    col_scale = 10.0 ** col_index
    row_scale = 100.0 ** row_index
    jitter = jnp.exp(jax.random.uniform(key_two, (rows, cols), jnp.float32, -0.69, 0.69))
    return row_scale[:, None] * col_scale[None, :] * jitter


def draw_query_second(key, part):
    return second_moment_estimate(jax.random.fold_in(key, 11), PROJECTION_RANK, QUERY_LATENT)


def draw_latent_second(key, part):
    return second_moment_estimate(jax.random.fold_in(key, 12), PROJECTION_RANK, KEY_VALUE_LATENT)


def spiked(values, key, source, target, blocks, factor):
    owner, partner = [(jnp.arange(values.shape[position]) // (values.shape[position] // blocks)).reshape([-1 if axis == position else 1 for axis in range(values.ndim)]) for position in (source, target)]
    chosen = jax.random.permutation(key, blocks)[partner]
    strong = (owner == chosen) | (owner == (partner + blocks // 2) % blocks)
    return jnp.where(strong, factor * values, values)


def block_levels(key, shape, shards, low, top_value):
    factor_of, own = 1.0, jax.random.fold_in(key, 6)
    for dim, parts in shards:
        draws = jnp.exp(jax.random.uniform(jax.random.fold_in(own, dim), (parts,), jnp.float32, low / len(shards), top_value / len(shards)))
        factor_of = factor_of * jnp.repeat(draws, shape[dim] // parts).reshape([-1 if axis == dim else 1 for axis in range(len(shape))])
    return factor_of


def centred(key, shape, scale, bound, cuts=(), kind=jnp.bfloat16):
    result = jax.random.normal(key, shape, jnp.float32) * scale
    if len(cuts) > 0:
        result = block_levels(key, shape, cuts, -0.22, 0.18) * result
    return jnp.clip(result, min=-bound, max=bound).astype(kind)


def gaussian_with(own_key, dims, scale, limit, pieces, heavy, kind=jnp.bfloat16):
    result = scale * jax.random.normal(own_key, dims, jnp.float32)
    if pieces:
        result = result * block_levels(own_key, dims, pieces, -0.22, 0.18)
    return jnp.clip(spiked(result, jax.random.fold_in(own_key, 3), *heavy), -limit, limit).astype(kind)


def setup_inputs(seed: int = 0) -> dict:
    keys = jax.random.split(jax.random.key(seed), 11)
    return {
        "normed_input": gaussian_with(keys[0], (TOKEN_TOTAL, MODEL_WIDTH), 1.0, 12.0, ((0, 32),), (0, 1, 32, 2.75)),
        "query_latent_cotangent": centred(keys[1], (TOKEN_TOTAL, QUERY_LATENT), (TOKEN_TOTAL ** -0.5), 0.015625, ((0, 32), (1, 4))),
        "key_value_latent_cotangent": centred(keys[2], (TOKEN_TOTAL, KEY_VALUE_LATENT), (TOKEN_TOTAL ** -0.5), 0.015625, ((0, 32), (1, 4))),
        "row_factor": gaussian_with(keys[3], (MODEL_WIDTH, PROJECTION_RANK), MODEL_WIDTH ** -0.5, 0.25, ((0, 32),), (0, 1, 32, 2.75)),
        "query_down_weight": centred(keys[4], (MODEL_WIDTH, QUERY_LATENT), 1.0, 6.0, ((0, 32), (1, 4)), jnp.float32),
        "key_value_down_weight": centred(keys[5], (MODEL_WIDTH, KEY_VALUE_LATENT), 1.0, 6.0, ((0, 32), (1, 4)), jnp.float32),
        "query_first_moment": centred(keys[6], (PROJECTION_RANK, QUERY_LATENT), 1.0, 6.0, ((0, 32), (1, 4)), jnp.float32),
        "key_value_first_moment": centred(keys[7], (PROJECTION_RANK, KEY_VALUE_LATENT), 1.0, 6.0, ((0, 32), (1, 4)), jnp.float32),
        "query_second": draw_query_second(jax.random.fold_in(keys[10], 71), 0),
        "latent_second": draw_latent_second(jax.random.fold_in(keys[10], 71), 0),
    }


def token_sum(left, right):
    return lax.dot_general(left, right, (((0,), (0,)), ((), ())), preferred_element_type=jnp.float32)

def update_one(gradient, factor32, weight, first, second):
    projected = jnp.dot(factor32.T, gradient, precision=lax.Precision.HIGHEST)
    first_new = 0.8 * first + 0.2 * projected
    second_new = 0.9 * second + 0.1 * projected * projected
    direction = first_new / (jnp.sqrt(second_new) + 1e-08)
    count = direction.shape[0] * direction.shape[1]
    scale = 0.5 * jnp.sqrt(jnp.float32(count)) / jnp.sqrt(jnp.sum(direction * direction) + 1e-06)
    step = jnp.dot(factor32, scale * direction, precision=lax.Precision.HIGHEST)
    weight_new = weight - step
    return (weight_new, step, weight_new.astype(jnp.bfloat16), first_new, second_new)

def reference(normed_input, query_latent_cotangent, key_value_latent_cotangent, row_factor, query_down_weight, key_value_down_weight, query_first_moment, key_value_first_moment, query_second, latent_second):
    factor32 = row_factor.astype(jnp.float32)
    grad_q = token_sum(normed_input, query_latent_cotangent)
    grad_kv = token_sum(normed_input, key_value_latent_cotangent)
    qn, qs, qc, qf, qv = update_one(grad_q, factor32, query_down_weight, query_first_moment, query_second)
    kn, ks, kc, kf, kv = update_one(grad_kv, factor32, key_value_down_weight, key_value_first_moment, latent_second)
    return (qn, kn, qs, ks, qc, kc, qf, kf, qv, kv)
```

```python
import functools

import jax
import jax.numpy as jnp
from jax import lax
from jax.experimental import pallas as pl
from jax.experimental.pallas import tpu as pltpu
from jax.sharding import PartitionSpec as P

MESH = pl.DeviceIdType.MESH
Z, Y, CORES, TP = 4, 4, 2, 4
FS = Z * Y * CORES
BF16, F32 = jnp.bfloat16, jnp.float32


def remote(src, dst, send, recv, **where):
    return pltpu.make_async_remote_copy(
        src_ref=src, dst_ref=dst, send_sem=send, recv_sem=recv, device_id=where, device_id_type=MESH
    )


def exchange_kernel(
    chunk,
    x_hbm, cq_hbm, ck_hbm, f_hbm, wq_hbm, wk_hbm, mq_hbm, mk_hbm, vq_hbm, vk_hbm,
    f_all, w_all, d_all, squares, total,
    x, cq, ck, ct, grad, gradh, wq, wk, mq, mk, vq, vk, part, parts,
    x_sem, small_sem, f_sem, gather_send, gather_recv, sum_sem, dir_sem, tp_sem,
):
    steps = x.shape[0] // chunk
    kv, qw = ck.shape[1], cq.shape[1]
    width = kv + qw
    me = lax.axis_index("fs")
    tp = lax.axis_index("tp")
    z, y, c = me // (Y * CORES), (me // CORES) % Y, me % CORES

    barrier = pltpu.get_barrier_semaphore()

    @pl.loop(1, FS)
    def _(d):
        pl.semaphore_signal(barrier, 1, device_id={"fs": (me + d) % FS}, device_id_type=MESH)

    @pl.loop(1, TP)
    def _(d):
        pl.semaphore_signal(barrier, 1, device_id={"tp": (tp + d) % TP}, device_id_type=MESH)

    own_f = pltpu.make_async_copy(f_hbm, f_all.at[z, y, c], f_sem)
    own_f.start()
    small = [
        pltpu.make_async_copy(a, b, small_sem.at[i])
        for i, (a, b) in enumerate(
            ((wq_hbm, wq), (wk_hbm, wk), (mq_hbm, mq), (mk_hbm, mk), (vq_hbm, vq), (vk_hbm, vk))
        )
    ]
    for copy in small[:2]:
        copy.start()

    def chunk_copies(k):
        rows = pl.ds(pl.multiple_of(k * chunk, chunk), chunk)
        return [
            pltpu.make_async_copy(a.at[rows], b.at[rows], x_sem.at[k, i])
            for i, (a, b) in enumerate(((cq_hbm, cq), (ck_hbm, ck), (x_hbm, x)))
        ]

    @pl.loop(0, steps)
    def _(k):
        for copy in chunk_copies(k):
            copy.start()

    for copy in small[2:]:
        copy.start()
    grad[...] = jnp.zeros_like(grad)
    own_f.wait()
    small[0].wait()
    small[1].wait()
    w_all[z, y, c, :, :kv] = wk[...].astype(BF16)
    w_all[z, y, c, :, kv:width] = wq[...].astype(BF16)
    pl.semaphore_wait(barrier, FS + TP - 2)

    half = f_all.shape[3] // 2
    lower, upper = pl.ds(0, half), pl.ds(half, half)
    stage_sem = lambda stage, which, lane: (
        gather_send.at[stage, which, lane],
        gather_recv.at[stage, which, lane],
    )
    peer_y = lambda d: (z * Y + (y + d) % Y) * CORES + c
    peer_z = lambda d: ((z + d) % Z * Y + y) * CORES + c

    def first_stage(a, which):
        for d in range(1, Y):
            block = a.at[z, y, c, lower]
            remote(block, block, *stage_sem(0, which, 0), fs=peer_y(d)).start()
        for d in range(1, Z):
            block = a.at[z, y, c, upper]
            remote(block, block, *stage_sem(0, which, 1), fs=peer_z(d)).start()

    def first_wait(a, which):
        seen = a.at[0, pl.ds(0, Y - 1), c, lower]
        remote(seen, seen, *stage_sem(0, which, 0), fs=peer_y(1)).wait()
        seen = a.at[pl.ds(0, Z - 1), 0, c, upper]
        remote(seen, seen, *stage_sem(0, which, 1), fs=peer_z(1)).wait()

    def second_stage(a, which):
        for d in range(1, Z):
            block = a.at[z, :, c, lower]
            remote(block, block, *stage_sem(1, which, 0), fs=peer_z(d)).start()
        for d in range(1, Y):
            block = a.at[:, y, c, upper]
            remote(block, block, *stage_sem(1, which, 1), fs=peer_y(d)).start()

    def second_wait(a, which):
        seen = a.at[pl.ds(0, Z - 1), :, c, lower]
        remote(seen, seen, *stage_sem(1, which, 0), fs=peer_z(1)).wait()
        seen = a.at[:, pl.ds(0, Y - 1), c, upper]
        remote(seen, seen, *stage_sem(1, which, 1), fs=peer_y(1)).wait()

    def partner_stage(a, which):
        block = a.at[:, :, c]
        remote(block, block, *stage_sem(2, which, 0), fs=me + 1 - 2 * c).start()

    def partner_wait(a, which):
        block = a.at[:, :, c]
        remote(block, block, *stage_sem(2, which, 0), fs=me + 1 - 2 * c).wait()

    first_stage(f_all, 0)
    first_stage(w_all, 1)

    @pl.loop(0, steps)
    def _(k):
        for copy in chunk_copies(k):
            copy.wait()
        rows = pl.ds(pl.multiple_of(k * chunk, chunk), chunk)
        ct[:kv, :] = ck[rows, :].T
        ct[kv:width, :] = cq[rows, :].T
        grad[...] += jnp.dot(ct[...], x[rows, :], preferred_element_type=F32)

        @pl.when(k == 3)
        def _():
            first_wait(f_all, 0)
            second_stage(f_all, 0)
            first_wait(w_all, 1)
            second_stage(w_all, 1)

    gradh[...] = grad[...].astype(BF16)
    second_wait(f_all, 0)
    partner_stage(f_all, 0)
    second_wait(w_all, 1)
    partner_stage(w_all, 1)
    partner_wait(f_all, 0)
    projected = jnp.dot(
        gradh[...], f_all[...].reshape(gradh.shape[1], f_all.shape[-1]), preferred_element_type=F32
    )
    rank = projected.shape[1] // FS
    part[:, :, :width] = projected.T.reshape(FS, rank, width).astype(BF16)

    @pl.loop(1, FS)
    def _(d):
        to = (me + d) % FS
        remote(part.at[to], parts.at[d - 1], sum_sem.at[0], sum_sem.at[1], fs=to).start()

    for copy in small[2:]:
        copy.wait()
    seen = parts
    remote(seen, seen, sum_sem.at[0], sum_sem.at[1], fs=me + 1 - 2 * c).wait()
    summed = part[me].astype(F32) + parts[...].astype(F32).sum(axis=0)
    total[...] = summed
    for low, high, first, second in ((0, kv, mk, vk), (kv, width, mq, vq)):
        got = summed[:, low:high]
        first_new = 0.8 * first[...] + 0.2 * got
        second_new = 0.9 * second[...] + 0.1 * got * got
        d_all[me, :, low:high] = (first_new / (jnp.sqrt(second_new) + 1e-08)).astype(BF16)

    @pl.loop(1, FS)
    def _(d):
        mine = d_all.at[me]
        remote(mine, mine, dir_sem.at[0], dir_sem.at[1], fs=(me + d) % FS).start()

    partner_wait(w_all, 1)
    seen = d_all.at[pl.ds(0, FS - 1)]
    remote(seen, seen, dir_sem.at[0], dir_sem.at[1], fs=me + 1 - 2 * c).wait()
    every = d_all[...].astype(F32)
    every = every * every
    sum_kv = jnp.sum(every[:, :, :kv], axis=(0, 1, 2), keepdims=True)[0]
    sum_q = jnp.sum(every[:, :, kv:width], axis=(0, 1, 2), keepdims=True)[0]
    which = lax.broadcasted_iota(jnp.int32, squares.shape[1:], 0)
    squares[tp] = jnp.where(which == 0, sum_kv, sum_q)

    @pl.loop(1, TP)
    def _(d):
        mine = squares.at[tp]
        remote(mine, mine, tp_sem.at[0], tp_sem.at[1], tp=(tp + d) % TP).start()

    seen = squares.at[pl.ds(0, TP - 1)]
    remote(seen, seen, tp_sem.at[0], tp_sem.at[1], tp=(tp + 1) % TP).wait()


def update_kernel(
    counts,
    f_all, w_all, d_all, squares, total, f_own, wq, wk, mq, mk, vq, vk,
    q_new, l_new, q_step, l_step, q_copy, l_copy, q_first, l_first, q_second, l_second,
):
    kv = wk.shape[1]
    width = kv + wq.shape[1]
    sums = squares[0] + squares[1] + squares[2] + squares[3]
    scales = [
        0.5 * jnp.sqrt(jnp.full((1, 1), counts[i], F32)) / jnp.sqrt(sums[i : i + 1, :1] + 1e-06)
        for i in range(2)
    ]
    summed = total[...]
    for low, high, first, second, first_new, second_new in (
        (0, kv, mk, vk, l_first, l_second),
        (kv, width, mq, vq, q_first, q_second),
    ):
        got = summed[:, low:high]
        first_new[...] = 0.8 * first[...] + 0.2 * got
        second_new[...] = 0.9 * second[...] + 0.1 * got * got
    rank = f_all.shape[-1]
    rows = 1
    for n in f_all.shape[:-1]:
        rows *= n
    directions = d_all[...].astype(F32).reshape(rank, d_all.shape[-1])[:, :width].astype(BF16)
    own = jnp.dot(f_own[...], directions, preferred_element_type=F32)
    for low, high, scale, weight, new, step in (
        (0, kv, scales[0], wk, l_new, l_step),
        (kv, width, scales[1], wq, q_new, q_step),
    ):
        taken = own[:, low:high] * scale
        step[...] = taken
        new[...] = weight[...] - taken
    whole = jnp.dot(f_all[...].reshape(rows, rank), directions, preferred_element_type=F32)
    weights = w_all[...].reshape(rows, w_all.shape[-1])
    l_copy[...] = (weights[:, :kv].astype(F32) - whole[:, :kv] * scales[0]).astype(BF16)
    q_copy[...] = (weights[:, kv:width].astype(F32) - whole[:, kv:] * scales[1]).astype(BF16)


def body(x, cq, ck, f, wq, wk, mq, mk, vq, vk):
    tokens, model = x.shape
    rows, rank = f.shape
    qw, kv = cq.shape[1], ck.shape[1]
    width = kv + qw
    lanes = -(-width // 128) * 128
    mine = rank // FS
    chunk = 512
    steps = tokens // chunk
    anywhere = pl.BlockSpec(memory_space=pl.ANY)
    vmem = pl.BlockSpec(memory_space=pltpu.VMEM)
    shape = jax.ShapeDtypeStruct
    dma = pltpu.SemaphoreType.DMA
    gathered = pl.pallas_call(
        functools.partial(exchange_kernel, chunk),
        out_shape=(
            shape((Z, Y, CORES, rows, rank), BF16),
            shape((Z, Y, CORES, rows, lanes), BF16),
            shape((FS, mine, lanes), BF16),
            shape((TP, 8, 128), F32),
            shape((mine, lanes), F32),
        ),
        in_specs=[anywhere] * 10,
        out_specs=(vmem,) * 5,
        scratch_shapes=[
            pltpu.VMEM((tokens, model), BF16),
            pltpu.VMEM((tokens, qw), BF16),
            pltpu.VMEM((tokens, kv), BF16),
            pltpu.VMEM((width, chunk), BF16),
            pltpu.VMEM((width, model), F32),
            pltpu.VMEM((width, model), BF16),
            pltpu.VMEM((rows, qw), F32),
            pltpu.VMEM((rows, kv), F32),
            pltpu.VMEM((mine, qw), F32),
            pltpu.VMEM((mine, kv), F32),
            pltpu.VMEM((mine, qw), F32),
            pltpu.VMEM((mine, kv), F32),
            pltpu.VMEM((FS, mine, lanes), BF16),
            pltpu.VMEM((FS - 1, mine, lanes), BF16),
            dma((steps, 3)),
            dma((6,)),
            dma,
            dma((3, 2, 2)),
            dma((3, 2, 2)),
            dma((2,)),
            dma((2,)),
            dma((2,)),
        ],
        compiler_params=pltpu.CompilerParams(
            collective_id=0, has_side_effects=True, vmem_limit_bytes=44 * 1024 * 1024
        ),
        name="exchange",
    )(x, cq, ck, f, wq, wk, mq, mk, vq, vk)
    counts = (rank * kv * TP, rank * qw * TP)
    model_rows = rows * FS
    lik = lambda a: shape(a.shape, a.dtype)
    return pl.pallas_call(
        functools.partial(update_kernel, counts),
        out_shape=(
            lik(wq), lik(wk), lik(wq), lik(wk),
            shape((model_rows, qw), BF16), shape((model_rows, kv), BF16),
            lik(mq), lik(mk), lik(vq), lik(vk),
        ),
        in_specs=[vmem] * 12,
        out_specs=(vmem,) * 10,
        name="update",
    )(*gathered[:4], gathered[4][:, :width], f, wq, wk, mq, mk, vq, vk)


def solution(mesh):
    return jax.shard_map(
        body,
        mesh=mesh,
        in_specs=(P("fs", None), P("fs", "tp"), P("fs", "tp"), P("fs", None)) + (P("fs", "tp"),) * 6,
        out_specs=(P("fs", "tp"),) * 4 + (P(None, "tp"),) * 2 + (P("fs", "tp"),) * 4,
        check_vma=False,
    )
```

```python
import functools

import jax
import jax.numpy as jnp
from jax import lax
from jax.experimental import pallas as pl
from jax.experimental.pallas import tpu as pltpu
from jax.sharding import PartitionSpec as P

MESH = pl.DeviceIdType.MESH
Z, Y, CORES, TP = 4, 4, 2, 4
FS = Z * Y * CORES
BF16, F32 = jnp.bfloat16, jnp.float32
CHUNK = 768
NEAR_AT, FAR_AT, W_NEAR_AT, W_FAR_AT, PAIR_AT = 3, 3, 4, 5, 5
SELF = 20
NEAREST = sorted(range(FS), key=lambda i: min(i // 8, 4 - i // 8) + min(i // 2 % 4, 4 - i // 2 % 4))


def remote(src, dst, send, recv, **where):
    return pltpu.make_async_remote_copy(
        src_ref=src, dst_ref=dst, send_sem=send, recv_sem=recv, device_id=where, device_id_type=MESH
    )


def exchange_kernel(
    x_hbm, cq_hbm, ck_hbm, f_hbm, wq_hbm, wk_hbm, mq_hbm, mk_hbm, vq_hbm, vk_hbm,
    w_all, q_weights, l_steps, q_steps, own_steps, squares, total,
    f_all, d_all, x, ck, ct, grad, gradh, wq, wk, mq, mk, vq, vk, part, parts,
    x_sem, small_sem, f_sem, own_send, own_recv, relay_send, relay_recv, pair_sem, sum_sem, dir_sem, square_sem,
):
    kv, qw = ck.shape[1], cq_hbm.shape[0]
    width = kv + qw
    me = lax.axis_index("fs")
    tp = lax.axis_index("tp")
    z, y, c = me // (Y * CORES), (me // CORES) % Y, me % CORES
    at = lambda dz, dy, dc: (((z + dz) % Z) * Y + (y + dy) % Y) * CORES + (c + dc) % CORES
    partner = at(0, 0, 1)

    def plane(i):
        return at((2 + i // (Y * CORES)) % Z, (2 + i // CORES) % Y, i % CORES)

    def to_plane(send):
        @pl.loop(0, FS)
        def _(i):
            pl.when(i != SELF)(functools.partial(send, i))

    barrier = pltpu.get_barrier_semaphore()
    axis_peers = [at(0, d, 0) for d in range(1, Y)] + [at(d, 0, 0) for d in range(1, Z)] + [partner]
    for peer in axis_peers:
        pl.semaphore_signal(barrier, 1, device_id={"fs": peer}, device_id_type=MESH)
    for d in range(1, TP):
        pl.semaphore_signal(barrier, 1, device_id={"tp": (tp + d) % TP}, device_id_type=MESH)

    own_f = pltpu.make_async_copy(f_hbm, f_all.at[z, y, c], f_sem)
    own_f.start()
    small = [
        pltpu.make_async_copy(a, b, small_sem.at[i])
        for i, (a, b) in enumerate(
            ((wq_hbm, wq), (wk_hbm, wk), (mq_hbm, mq), (mk_hbm, mk), (vq_hbm, vq), (vk_hbm, vk))
        )
    ]
    for copy in small[:2]:
        copy.start()

    steps = x.shape[0] // CHUNK
    span = lambda k: pl.ds(pl.multiple_of(k * CHUNK, CHUNK), CHUNK)
    cq_copy = lambda k: pltpu.make_async_copy(
        cq_hbm.at[:, span(k)], ct.at[pl.ds(kv, qw), span(k)], x_sem.at[k, 0]
    )
    ck_copy = lambda k: pltpu.make_async_copy(ck_hbm.at[span(k)], ck.at[span(k)], x_sem.at[k, 1])
    x_copy = lambda k: pltpu.make_async_copy(x_hbm.at[span(k)], x.at[span(k)], x_sem.at[k, 2])

    @pl.loop(0, steps)
    def _(k):
        ck_copy(k).start()
        cq_copy(k).start()
        x_copy(k).start()

    for copy in small[2:]:
        copy.start()

    lower, upper = pl.ds(0, f_all.shape[3] // 2), pl.ds(f_all.shape[3] // 2, f_all.shape[3] // 2)

    def own_copy(a, which, along, d, slot):
        where = at(0, d, 0) if along else at(d, 0, 0)
        block = a.at[slot]
        return remote(
            block, block, own_send.at[which, along, d - 1], own_recv.at[which, along, d - 1], fs=where
        )

    def own_start(a, which):
        for d in (2, 1, 3):
            for along in range(2):
                own_copy(a, which, along, d, (z, y, c)).start()

    def relay_copy(a, which, along, d, e, slot):
        where = at(0, e, 0) if along else at(e, 0, 0)
        block = a.at[slot + ((upper if along else lower),)]
        return remote(
            block, block, relay_send.at[which, along], relay_recv.at[which, along], fs=where
        )

    def relay(a, which, distances):
        for d in distances:
            came_y = (z, (y - d + Y) % Y, c)
            came_z = ((z - d + Z) % Z, y, c)
            own_copy(a, which, 1, d, came_y).wait_recv()
            own_copy(a, which, 0, d, came_z).wait_recv()
            for e in (2, 1, 3):
                relay_copy(a, which, 0, d, e, came_y).start()
                relay_copy(a, which, 1, d, e, came_z).start()

    def relay_wait(a, which):
        for along in range(2):
            seen = a.at[pl.ds(0, 3), pl.ds(0, 3), c, lower]
            remote(seen, seen, relay_send.at[which, along], relay_recv.at[which, along], fs=partner).wait()
        for d in (1, 2, 3):
            for along in range(2):
                own_copy(a, which, along, d, (z, y, c)).wait_send()

    def pair_copy(a, which):
        block = a.at[:, :, c]
        return remote(block, block, pair_sem.at[which, 0], pair_sem.at[which, 1], fs=partner)

    def pair_start(a, which):
        relay_wait(a, which)
        pair_copy(a, which).start()

    own_f.wait()
    pl.semaphore_wait(barrier, len(axis_peers) + TP - 1)
    own_start(f_all, 0)
    small[0].wait()
    small[1].wait()
    w_all[z, y, c, :, :kv] = wk[...].astype(BF16)
    w_all[z, y, c, :, kv:width] = wq[...].astype(BF16)
    grad[...] = jnp.zeros_like(grad)
    own_start(w_all, 1)

    @pl.loop(0, steps)
    def _(k):
        for step, a, which, distances in (
            (NEAR_AT, f_all, 0, (1, 3)),
            (FAR_AT, f_all, 0, (2,)),
            (W_NEAR_AT, w_all, 1, (1, 3)),
            (W_FAR_AT, w_all, 1, (2,)),
        ):
            pl.when(k == step)(functools.partial(relay, a, which, distances))
        pl.when(k == PAIR_AT)(functools.partial(pair_start, f_all, 0))
        ck_copy(k).wait()
        cq_copy(k).wait()
        x_copy(k).wait()
        ct[:kv, span(k)] = ck[span(k), :].T
        grad[...] += jnp.dot(ct[:, span(k)], x[span(k), :], preferred_element_type=F32)

    gradh[...] = grad[...].astype(BF16)
    pair_copy(f_all, 0).wait()
    projected = jnp.dot(
        gradh[...], f_all[...].reshape(gradh.shape[1], f_all.shape[-1]), preferred_element_type=F32
    )
    rank = projected.shape[1] // FS
    part[:, :, :width] = projected.T.reshape(FS, rank, width).astype(BF16)

    @to_plane
    def _(i):
        to = plane(i)
        remote(part.at[to], parts.at[i], sum_sem.at[0], sum_sem.at[1], fs=to).start()

    pair_start(w_all, 1)
    for copy in small[2:]:
        copy.wait()
    seen = parts.at[pl.ds(0, FS - 1)]
    remote(seen, seen, sum_sem.at[0], sum_sem.at[1], fs=partner).wait()
    parts[SELF] = part[me]
    summed = parts[...].astype(F32).sum(axis=0)
    total[...] = summed
    for low, high, first, second in ((0, kv, mk, vk), (kv, width, mq, vq)):
        got = summed[:, low:high]
        first_new = 0.8 * first[...] + 0.2 * got
        second_new = 0.9 * second[...] + 0.1 * got * got
        direction = first_new / (jnp.sqrt(second_new) + 1e-08)
        d_all[me, :, low:high] = direction.astype(BF16)
    mine = d_all.at[me]

    for peer in NEAREST:

        @pl.when(me != peer)
        def _():
            remote(mine, mine, dir_sem.at[0], dir_sem.at[1], fs=peer).start()

    seen = d_all.at[pl.ds(0, FS - 1)]
    remote(seen, seen, dir_sem.at[0], dir_sem.at[1], fs=partner).wait()
    every = d_all[...].astype(F32).reshape(FS * rank, d_all.shape[-1])[:, :width]
    lengths = jnp.sum(every * every, axis=0, keepdims=True)
    lane = lax.broadcasted_iota(jnp.int32, (1, 128), 1)
    squares[tp] = jnp.where(
        lane < 64,
        jnp.sum(lengths[:, :kv], axis=1, keepdims=True),
        jnp.sum(lengths[:, kv:], axis=1, keepdims=True),
    )
    mine = squares.at[tp]
    for d in (2, 1, 3):
        remote(mine, mine, square_sem.at[0], square_sem.at[1], tp=(tp + d) % TP).start()
    factor = f_all[...].reshape(l_steps.shape[0], f_all.shape[-1])
    directions = every.astype(BF16)
    own_steps[...] = jnp.dot(f_all[z, y, c], directions, preferred_element_type=F32)
    l_steps[...] = jnp.dot(factor, directions[:, :kv], preferred_element_type=F32)
    q_steps[...] = lax.dot_general(
        directions[:, kv:], factor, (((0,), (1,)), ((), ())), preferred_element_type=F32
    )
    pair_copy(w_all, 1).wait()
    q_weights[...] = w_all[...].reshape(l_steps.shape[0], w_all.shape[-1])[:, kv:width].T
    seen = squares.at[pl.ds(0, TP - 1)]
    remote(seen, seen, square_sem.at[0], square_sem.at[1], tp=(tp + 1) % TP).wait()


def update_kernel(
    counts,
    w_all, q_weights, l_steps, q_steps, own_steps, squares, total, wq, wk, mq, mk, vq, vk,
    q_new, l_new, q_step, l_step, q_copy, l_copy, q_first, l_first, q_second, l_second,
):
    kv = wk.shape[1]
    width = kv + wq.shape[1]
    sums = squares[0] + squares[1] + squares[2] + squares[3]
    scales = [
        0.5 * jnp.sqrt(jnp.full((1, 1), counts[i], F32)) / jnp.sqrt(sums[:, 64 * i : 64 * i + 1] + 1e-06)
        for i in range(2)
    ]
    summed = total[...]
    for low, high, first, second, first_new, second_new in (
        (0, kv, mk, vk, l_first, l_second),
        (kv, width, mq, vq, q_first, q_second),
    ):
        got = summed[:, low:high]
        first_new[...] = 0.8 * first[...] + 0.2 * got
        second_new[...] = 0.9 * second[...] + 0.1 * got * got
    own = own_steps[...]
    for low, high, scale, weight, new, step in (
        (0, kv, scales[0], wk, l_new, l_step),
        (kv, width, scales[1], wq, q_new, q_step),
    ):
        taken = own[:, low:high] * scale
        step[...] = taken
        new[...] = weight[...] - taken
    weights = w_all[...].reshape(l_steps.shape[0], w_all.shape[-1])
    l_copy[...] = (weights[:, :kv].astype(F32) - l_steps[...] * scales[0]).astype(BF16)
    q_copy[...] = (q_weights[...].astype(F32) - q_steps[...] * scales[1]).astype(BF16)


def body(x, cq, ck, f, wq, wk, mq, mk, vq, vk):
    tokens, model = x.shape
    rows, rank = f.shape
    qw, kv = cq.shape[1], ck.shape[1]
    width = kv + qw
    lanes = -(-width // 128) * 128
    mine = rank // FS
    hbm = pl.BlockSpec(memory_space=pltpu.HBM)
    vmem = pl.BlockSpec(memory_space=pltpu.VMEM)
    shape = jax.ShapeDtypeStruct
    dma = pltpu.SemaphoreType.DMA
    gathered = pl.pallas_call(
        exchange_kernel,
        out_shape=(
            shape((Z, Y, CORES, rows, lanes), BF16),
            shape((qw, FS * rows), BF16),
            shape((FS * rows, kv), F32),
            shape((qw, FS * rows), F32),
            shape((rows, width), F32),
            shape((TP, 1, 128), F32),
            shape((mine, lanes), F32),
        ),
        in_specs=[hbm] * 10,
        out_specs=(vmem,) * 7,
        scratch_shapes=[
            pltpu.VMEM((Z, Y, CORES, rows, rank), BF16),
            pltpu.VMEM((FS, mine, lanes), BF16),
            pltpu.VMEM((tokens, model), BF16),
            pltpu.VMEM((tokens, kv), BF16),
            pltpu.VMEM((width, tokens), BF16),
            pltpu.VMEM((width, model), F32),
            pltpu.VMEM((width, model), BF16),
            pltpu.VMEM((rows, qw), F32),
            pltpu.VMEM((rows, kv), F32),
            pltpu.VMEM((mine, qw), F32),
            pltpu.VMEM((mine, kv), F32),
            pltpu.VMEM((mine, qw), F32),
            pltpu.VMEM((mine, kv), F32),
            pltpu.VMEM((FS, mine, lanes), BF16),
            pltpu.VMEM((FS, mine, lanes), BF16),
            dma((tokens // CHUNK, 3)),
            dma((6,)),
            dma,
            dma((2, 2, 3)),
            dma((2, 2, 3)),
            dma((2, 2)),
            dma((2, 2)),
            dma((2, 2)),
            dma((2,)),
            dma((2,)),
            dma((2,)),
        ],
        compiler_params=pltpu.CompilerParams(
            collective_id=0, has_side_effects=True, vmem_limit_bytes=44 * 1024 * 1024
        ),
        name="exchange",
    )(*(pltpu.with_memory_space_constraint(a, pltpu.HBM) for a in (x, cq.T, ck, f, wq, wk, mq, mk, vq, vk)))
    counts = (rank * kv * TP, rank * qw * TP)
    model_rows = rows * FS
    like = lambda a: shape(a.shape, a.dtype)
    outs = pl.pallas_call(
        functools.partial(update_kernel, counts),
        out_shape=(
            like(wq), like(wk), like(wq), like(wk),
            shape((qw, model_rows), BF16), shape((model_rows, kv), BF16),
            like(mq), like(mk), like(vq), like(vk),
        ),
        in_specs=[vmem] * 13,
        out_specs=(vmem,) * 10,
        compiler_params=pltpu.CompilerParams(vmem_limit_bytes=16 * 1024 * 1024),
        name="update",
    )(*gathered, wq, wk, mq, mk, vq, vk)
    return outs[:4] + (outs[4].T,) + outs[5:]


def solution(mesh):
    return jax.shard_map(
        body,
        mesh=mesh,
        in_specs=(P("fs", None), P("fs", "tp"), P("fs", "tp"), P("fs", None)) + (P("fs", "tp"),) * 6,
        out_specs=(P("fs", "tp"),) * 4 + (P(None, "tp"),) * 2 + (P("fs", "tp"),) * 4,
        check_vma=False,
    )
```

```python
import functools

import jax
import jax.numpy as jnp
from jax import lax
from jax.experimental import pallas as pl
from jax.experimental.pallas import tpu as pltpu
from jax.sharding import PartitionSpec as P

MESH = pl.DeviceIdType.MESH
Z, Y, CORES, TP = 4, 4, 2, 4
FS = Z * Y * CORES
BF16, F32 = jnp.bfloat16, jnp.float32
CHUNK = 512
NEAR_AT, FAR_AT, PAIR_AT = 4, 4, 8
NEAREST = sorted(range(FS), key=lambda i: min(i // 8, 4 - i // 8) + min(i // 2 % 4, 4 - i // 2 % 4))


FARTHEST = NEAREST[::-1]


def remote(src, dst, send, recv, **where):
    return pltpu.make_async_remote_copy(
        src_ref=src, dst_ref=dst, send_sem=send, recv_sem=recv, device_id=where, device_id_type=MESH
    )


def exchange_kernel(
    x_hbm, cq_hbm, ck_hbm, f_hbm, wq_hbm, wk_hbm, mq_hbm, mk_hbm, vq_hbm, vk_hbm,
    w_all, q_weights, l_steps, q_steps, own_steps, squares, total,
    f_all, d_all, x, ck, ct, grad, wq, wk, mq, mk, vq, vk, part, parts,
    x_sem, small_sem, f_sem, own_send, own_recv, relay_send, relay_recv, pair_sem, sum_sem, dir_sem, square_sem,
):
    kv, qw = ck.shape[1], cq_hbm.shape[0]
    width = kv + qw
    me = lax.axis_index("fs")
    tp = lax.axis_index("tp")
    z, y, c = me // (Y * CORES), (me // CORES) % Y, me % CORES
    at = lambda dz, dy, dc: (((z + dz) % Z) * Y + (y + dy) % Y) * CORES + (c + dc) % CORES
    partner = at(0, 0, 1)

    barrier = pltpu.get_barrier_semaphore()
    axis_peers = [at(0, d, 0) for d in range(1, Y)] + [at(d, 0, 0) for d in range(1, Z)] + [partner]
    for peer in axis_peers:
        pl.semaphore_signal(barrier, 1, device_id={"fs": peer}, device_id_type=MESH)
    for d in range(1, TP):
        pl.semaphore_signal(barrier, 1, device_id={"tp": (tp + d) % TP}, device_id_type=MESH)

    own_f = pltpu.make_async_copy(f_hbm, f_all.at[z, y, c], f_sem)
    own_f.start()
    small = [
        pltpu.make_async_copy(a, b, small_sem.at[i])
        for i, (a, b) in enumerate(
            ((wq_hbm, wq), (wk_hbm, wk), (mq_hbm, mq), (mk_hbm, mk), (vq_hbm, vq), (vk_hbm, vk))
        )
    ]
    for copy in small[:2]:
        copy.start()

    steps = x.shape[0] // CHUNK
    span = lambda k: pl.ds(pl.multiple_of(k * CHUNK, CHUNK), CHUNK)
    cq_copy = lambda k: pltpu.make_async_copy(
        cq_hbm.at[:, span(k)], ct.at[pl.ds(kv, qw), span(k)], x_sem.at[k, 0]
    )
    ck_copy = lambda k: pltpu.make_async_copy(ck_hbm.at[span(k)], ck.at[span(k)], x_sem.at[k, 1])
    x_copy = lambda k: pltpu.make_async_copy(x_hbm.at[span(k)], x.at[span(k)], x_sem.at[k, 2])

    @pl.loop(0, steps)
    def _(k):
        ck_copy(k).start()
        cq_copy(k).start()
        x_copy(k).start()

    for copy in small[2:]:
        copy.start()

    lower, upper = pl.ds(0, f_all.shape[3] // 2), pl.ds(f_all.shape[3] // 2, f_all.shape[3] // 2)

    def own_copy(a, which, along, d, slot):
        where = at(0, d, 0) if along else at(d, 0, 0)
        block = a.at[slot]
        return remote(
            block, block, own_send.at[which, along, d - 1], own_recv.at[which, along, d - 1], fs=where
        )

    def own_start(a, which):
        for d in (2, 1, 3):
            for along in range(2):
                own_copy(a, which, along, d, (z, y, c)).start()

    def relay_copy(a, which, along, d, e, slot):
        where = at(0, e, 0) if along else at(e, 0, 0)
        block = a.at[slot + ((upper if along else lower),)]
        return remote(
            block, block, relay_send.at[which, along], relay_recv.at[which, along], fs=where
        )

    def relay(a, which, distances):
        for d in distances:
            came_y = (z, (y - d + Y) % Y, c)
            came_z = ((z - d + Z) % Z, y, c)
            own_copy(a, which, 1, d, came_y).wait_recv()
            own_copy(a, which, 0, d, came_z).wait_recv()
            for e in (2, 1, 3):
                relay_copy(a, which, 0, d, e, came_y).start()
                relay_copy(a, which, 1, d, e, came_z).start()

    def relay_wait(a, which):
        for along in range(2):
            seen = a.at[pl.ds(0, 3), pl.ds(0, 3), c, lower]
            remote(seen, seen, relay_send.at[which, along], relay_recv.at[which, along], fs=partner).wait()
        for d in (1, 2, 3):
            for along in range(2):
                own_copy(a, which, along, d, (z, y, c)).wait_send()

    def pair_copy(a, which):
        block = a.at[:, :, c]
        return remote(block, block, pair_sem.at[which, 0], pair_sem.at[which, 1], fs=partner)

    def pair_start(a, which):
        relay_wait(a, which)
        pair_copy(a, which).start()

    own_f.wait()
    pl.semaphore_wait(barrier, len(axis_peers) + TP - 1)
    own_start(f_all, 0)
    small[0].wait()
    small[1].wait()
    w_all[z, y, c, :, :kv] = wk[...].astype(BF16)
    w_all[z, y, c, :, kv:width] = wq[...].astype(BF16)
    grad[...] = jnp.zeros_like(grad)
    own_start(w_all, 1)

    @pl.loop(0, steps)
    def _(k):
        for step, a, which, distances in (
            (NEAR_AT, f_all, 0, (1, 3)),
            (FAR_AT, f_all, 0, (2,)),
        ):
            pl.when(k == step)(functools.partial(relay, a, which, distances))
        pl.when(k == PAIR_AT)(functools.partial(pair_start, f_all, 0))
        ck_copy(k).wait()
        cq_copy(k).wait()
        x_copy(k).wait()
        ct[:kv, span(k)] = ck[span(k), :].T
        grad[...] += jnp.dot(ct[:, span(k)], x[span(k), :], preferred_element_type=F32)

    pair_copy(f_all, 0).wait()
    projected = jnp.dot(
        grad[...].astype(BF16), f_all[...].reshape(grad.shape[1], f_all.shape[-1]), preferred_element_type=F32
    )
    rank = projected.shape[1] // FS
    part[:, :, :width] = projected.T.reshape(FS, rank, width).astype(BF16)

    for peer in FARTHEST:

        @pl.when(me != peer)
        def _():
            remote(part.at[peer], parts.at[me], sum_sem.at[0], sum_sem.at[1], fs=peer).start()

    relay(w_all, 1, (1, 3, 2))
    for copy in small[2:]:
        copy.wait()
    seen = parts.at[pl.ds(0, FS - 1)]
    remote(seen, seen, sum_sem.at[0], sum_sem.at[1], fs=partner).wait()
    parts[me] = part[me]
    summed = parts[...].astype(F32).sum(axis=0)
    total[...] = summed
    for low, high, first, second in ((0, kv, mk, vk), (kv, width, mq, vq)):
        got = summed[:, low:high]
        first_new = 0.8 * first[...] + 0.2 * got
        second_new = 0.9 * second[...] + 0.1 * got * got
        direction = first_new / (jnp.sqrt(second_new) + 1e-08)
        d_all[me, :, low:high] = direction.astype(BF16)
    mine = d_all.at[me]

    for peer in NEAREST:

        @pl.when(me != peer)
        def _():
            remote(mine, mine, dir_sem.at[0], dir_sem.at[1], fs=peer).start()

    pair_start(w_all, 1)
    seen = d_all.at[pl.ds(0, FS - 1)]
    remote(seen, seen, dir_sem.at[0], dir_sem.at[1], fs=partner).wait()
    every = d_all[...].astype(F32).reshape(FS * rank, d_all.shape[-1])[:, :width]
    lengths = jnp.sum(every * every, axis=0, keepdims=True)
    lane = lax.broadcasted_iota(jnp.int32, (1, 128), 1)
    squares[tp] = jnp.where(
        lane < 64,
        jnp.sum(lengths[:, :kv], axis=1, keepdims=True),
        jnp.sum(lengths[:, kv:], axis=1, keepdims=True),
    )
    mine = squares.at[tp]
    for d in (2, 1, 3):
        remote(mine, mine, square_sem.at[0], square_sem.at[1], tp=(tp + d) % TP).start()
    factor = f_all[...].reshape(l_steps.shape[0], f_all.shape[-1])
    directions = every.astype(BF16)
    own_steps[...] = jnp.dot(f_all[z, y, c], directions, preferred_element_type=F32)
    l_steps[...] = jnp.dot(factor, directions[:, :kv], preferred_element_type=F32)
    q_steps[...] = lax.dot_general(
        directions[:, kv:], factor, (((0,), (1,)), ((), ())), preferred_element_type=F32
    )
    pair_copy(w_all, 1).wait()
    q_weights[...] = w_all[...].reshape(l_steps.shape[0], w_all.shape[-1])[:, kv:width].T
    seen = squares.at[pl.ds(0, TP - 1)]
    remote(seen, seen, square_sem.at[0], square_sem.at[1], tp=(tp + 1) % TP).wait()


def update_kernel(
    counts,
    w_all, q_weights, l_steps, q_steps, own_steps, squares, total, wq, wk, mq, mk, vq, vk,
    q_new, l_new, q_step, l_step, q_copy, l_copy, q_first, l_first, q_second, l_second,
):
    kv = wk.shape[1]
    width = kv + wq.shape[1]
    sums = squares[0] + squares[1] + squares[2] + squares[3]
    scales = [
        0.5 * jnp.sqrt(jnp.full((1, 1), counts[i], F32)) / jnp.sqrt(sums[:, 64 * i : 64 * i + 1] + 1e-06)
        for i in range(2)
    ]
    summed = total[...]
    for low, high, first, second, first_new, second_new in (
        (0, kv, mk, vk, l_first, l_second),
        (kv, width, mq, vq, q_first, q_second),
    ):
        got = summed[:, low:high]
        first_new[...] = 0.8 * first[...] + 0.2 * got
        second_new[...] = 0.9 * second[...] + 0.1 * got * got
    own = own_steps[...]
    for low, high, scale, weight, new, step in (
        (0, kv, scales[0], wk, l_new, l_step),
        (kv, width, scales[1], wq, q_new, q_step),
    ):
        taken = own[:, low:high] * scale
        step[...] = taken
        new[...] = weight[...] - taken
    weights = w_all[...].reshape(l_steps.shape[0], w_all.shape[-1])
    l_copy[...] = (weights[:, :kv].astype(F32) - l_steps[...] * scales[0]).astype(BF16)
    q_copy[...] = (q_weights[...].astype(F32) - q_steps[...] * scales[1]).astype(BF16)


def body(x, cq, ck, f, wq, wk, mq, mk, vq, vk):
    tokens, model = x.shape
    rows, rank = f.shape
    qw, kv = cq.shape[1], ck.shape[1]
    width = kv + qw
    lanes = -(-width // 128) * 128
    mine = rank // FS
    hbm = pl.BlockSpec(memory_space=pltpu.HBM)
    vmem = pl.BlockSpec(memory_space=pltpu.VMEM)
    shape = jax.ShapeDtypeStruct
    dma = pltpu.SemaphoreType.DMA
    gathered = pl.pallas_call(
        exchange_kernel,
        out_shape=(
            shape((Z, Y, CORES, rows, lanes), BF16),
            shape((qw, FS * rows), BF16),
            shape((FS * rows, kv), F32),
            shape((qw, FS * rows), F32),
            shape((rows, width), F32),
            shape((TP, 1, 128), F32),
            shape((mine, lanes), F32),
        ),
        in_specs=[hbm] * 10,
        out_specs=(vmem,) * 7,
        scratch_shapes=[
            pltpu.VMEM((Z, Y, CORES, rows, rank), BF16),
            pltpu.VMEM((FS, mine, lanes), BF16),
            pltpu.VMEM((tokens, model), BF16),
            pltpu.VMEM((tokens, kv), BF16),
            pltpu.VMEM((width, tokens), BF16),
            pltpu.VMEM((width, model), F32),
            pltpu.VMEM((rows, qw), F32),
            pltpu.VMEM((rows, kv), F32),
            pltpu.VMEM((mine, qw), F32),
            pltpu.VMEM((mine, kv), F32),
            pltpu.VMEM((mine, qw), F32),
            pltpu.VMEM((mine, kv), F32),
            pltpu.VMEM((FS, mine, lanes), BF16),
            pltpu.VMEM((FS, mine, lanes), BF16),
            dma((tokens // CHUNK, 3)),
            dma((6,)),
            dma,
            dma((2, 2, 3)),
            dma((2, 2, 3)),
            dma((2, 2)),
            dma((2, 2)),
            dma((2, 2)),
            dma((2,)),
            dma((2,)),
            dma((2,)),
        ],
        compiler_params=pltpu.CompilerParams(
            collective_id=0, has_side_effects=True, vmem_limit_bytes=44 * 1024 * 1024
        ),
        name="exchange",
    )(*(pltpu.with_memory_space_constraint(a, pltpu.HBM) for a in (x, cq.T, ck, f, wq, wk, mq, mk, vq, vk)))
    counts = (rank * kv * TP, rank * qw * TP)
    model_rows = rows * FS
    like = lambda a: shape(a.shape, a.dtype)
    outs = pl.pallas_call(
        functools.partial(update_kernel, counts),
        out_shape=(
            like(wq), like(wk), like(wq), like(wk),
            shape((qw, model_rows), BF16), shape((model_rows, kv), BF16),
            like(mq), like(mk), like(vq), like(vk),
        ),
        in_specs=[vmem] * 13,
        out_specs=(vmem,) * 10,
        compiler_params=pltpu.CompilerParams(vmem_limit_bytes=16 * 1024 * 1024),
        name="update",
    )(*gathered, wq, wk, mq, mk, vq, vk)
    return outs[:4] + (outs[4].T,) + outs[5:]


def solution(mesh):
    return jax.shard_map(
        body,
        mesh=mesh,
        in_specs=(P("fs", None), P("fs", "tp"), P("fs", "tp"), P("fs", None)) + (P("fs", "tp"),) * 6,
        out_specs=(P("fs", "tp"),) * 4 + (P(None, "tp"),) * 2 + (P("fs", "tp"),) * 4,
        check_vma=False,
    )
```

```python
import functools

import jax
import jax.numpy as jnp
from jax import lax
from jax.experimental import pallas as pl
from jax.experimental.pallas import tpu as pltpu
from jax.sharding import PartitionSpec as P

MESH = pl.DeviceIdType.MESH
Z, Y, CORES, TP = 4, 4, 2, 4
FS = Z * Y * CORES
BF16, F32 = jnp.bfloat16, jnp.float32
CHUNK = 512
NEAR_AT, FAR_AT, PAIR_AT = 4, 4, 8
NEAREST = sorted(range(FS), key=lambda i: min(i // 8, 4 - i // 8) + min(i // 2 % 4, 4 - i // 2 % 4))


FARTHEST = NEAREST[::-1]


def remote(src, dst, send, recv, **where):
    return pltpu.make_async_remote_copy(
        src_ref=src, dst_ref=dst, send_sem=send, recv_sem=recv, device_id=where, device_id_type=MESH
    )


def exchange_kernel(
    x_hbm, cq_hbm, ck_hbm, f_hbm, wq_hbm, wk_hbm, mq_hbm, mk_hbm, vq_hbm, vk_hbm,
    w_all, q_weights, l_steps, q_steps, own_steps, squares, total,
    f_all, d_all, x, ck, ct, grad, wq, wk, mq, mk, vq, vk, part, parts, crossed, own_square,
    x_sem, small_sem, f_sem, own_send, own_recv, relay_send, relay_recv, pair_sem, sum_sem, dir_sem, square_sem,
):
    kv, qw = ck.shape[1], cq_hbm.shape[0]
    width = kv + qw
    me = lax.axis_index("fs")
    tp = lax.axis_index("tp")
    z, y, c = me // (Y * CORES), (me // CORES) % Y, me % CORES
    at = lambda dz, dy, dc: (((z + dz) % Z) * Y + (y + dy) % Y) * CORES + (c + dc) % CORES
    partner = at(0, 0, 1)

    barrier = pltpu.get_barrier_semaphore()
    axis_peers = [at(0, d, 0) for d in range(1, Y)] + [at(d, 0, 0) for d in range(1, Z)] + [partner]
    for peer in axis_peers:
        pl.semaphore_signal(barrier, 1, device_id={"fs": peer}, device_id_type=MESH)
    for d in range(1, TP):
        pl.semaphore_signal(barrier, 1, device_id={"tp": (tp + d) % TP}, device_id_type=MESH)

    own_f = pltpu.make_async_copy(f_hbm, f_all.at[z, y, c], f_sem)
    own_f.start()
    small = [
        pltpu.make_async_copy(a, b, small_sem.at[i])
        for i, (a, b) in enumerate(
            ((wq_hbm, wq), (wk_hbm, wk), (mq_hbm, mq), (mk_hbm, mk), (vq_hbm, vq), (vk_hbm, vk))
        )
    ]
    for copy in small[:2]:
        copy.start()

    steps = x.shape[0] // CHUNK
    span = lambda k: pl.ds(pl.multiple_of(k * CHUNK, CHUNK), CHUNK)
    cq_copy = lambda k: pltpu.make_async_copy(
        cq_hbm.at[:, span(k)], ct.at[pl.ds(kv, qw), span(k)], x_sem.at[k, 0]
    )
    ck_copy = lambda k: pltpu.make_async_copy(ck_hbm.at[span(k)], ck.at[span(k)], x_sem.at[k, 1])
    x_copy = lambda k: pltpu.make_async_copy(x_hbm.at[span(k)], x.at[span(k)], x_sem.at[k, 2])

    @pl.loop(0, steps)
    def _(k):
        ck_copy(k).start()
        cq_copy(k).start()
        x_copy(k).start()

    for copy in small[2:]:
        copy.start()

    lower, upper = pl.ds(0, f_all.shape[3] // 2), pl.ds(f_all.shape[3] // 2, f_all.shape[3] // 2)

    def own_copy(a, which, along, d, slot):
        where = at(0, d, 0) if along else at(d, 0, 0)
        block = a.at[slot]
        return remote(
            block, block, own_send.at[which, along, d - 1], own_recv.at[which, along, d - 1], fs=where
        )

    def own_start(a, which):
        for d in (2, 1, 3):
            for along in range(2):
                own_copy(a, which, along, d, (z, y, c)).start()

    def relay_copy(a, which, along, d, e, slot):
        where = at(0, e, 0) if along else at(e, 0, 0)
        block = a.at[slot + ((upper if along else lower),)]
        return remote(
            block, block, relay_send.at[which, along], relay_recv.at[which, along], fs=where
        )

    def relay(a, which, distances):
        for d in distances:
            came_y = (z, (y - d + Y) % Y, c)
            came_z = ((z - d + Z) % Z, y, c)
            own_copy(a, which, 1, d, came_y).wait_recv()
            own_copy(a, which, 0, d, came_z).wait_recv()
            for e in (2, 1, 3):
                relay_copy(a, which, 0, d, e, came_y).start()
                relay_copy(a, which, 1, d, e, came_z).start()

    def relay_wait(a, which):
        for along in range(2):
            seen = a.at[pl.ds(0, 3), pl.ds(0, 3), c, lower]
            remote(seen, seen, relay_send.at[which, along], relay_recv.at[which, along], fs=partner).wait()
        for d in (1, 2, 3):
            for along in range(2):
                own_copy(a, which, along, d, (z, y, c)).wait_send()

    def pair_copy(a, which):
        block = a.at[:, :, c]
        return remote(block, block, pair_sem.at[which, 0], pair_sem.at[which, 1], fs=partner)

    def pair_start(a, which):
        relay_wait(a, which)
        pair_copy(a, which).start()

    def pair_block(a, which, dz, dy):
        block = a.at[(z + dz) % Z, (y + dy) % Y, c]
        return remote(block, block, pair_sem.at[which, 0], pair_sem.at[which, 1], fs=partner)

    def pair_early(a, which):
        for d in range(4):
            pair_block(a, which, 0, d).start()
        for d in range(1, 4):
            pair_block(a, which, d, 0).start()

    def pair_late(a, which):
        relay_wait(a, which)
        for dz in range(1, 4):
            for dy in range(1, 4):
                pair_block(a, which, dz, dy).start()

    own_f.wait()
    pl.semaphore_wait(barrier, len(axis_peers) + TP - 1)
    own_start(f_all, 0)
    small[0].wait()
    small[1].wait()
    w_all[z, y, c, :, :kv] = wk[...].astype(BF16)
    w_all[z, y, c, :, kv:width] = wq[...].astype(BF16)
    grad[...] = jnp.zeros_like(grad)
    own_start(w_all, 1)

    @pl.loop(0, steps)
    def _(k):
        for step, a, which, distances in (
            (NEAR_AT, f_all, 0, (1, 3)),
            (FAR_AT, f_all, 0, (2,)),
        ):
            pl.when(k == step)(functools.partial(relay, a, which, distances))
        pl.when(k == PAIR_AT - 2)(functools.partial(pair_early, f_all, 0))
        pl.when(k == PAIR_AT)(functools.partial(pair_late, f_all, 0))
        ck_copy(k).wait()
        cq_copy(k).wait()
        x_copy(k).wait()
        ct[:kv, span(k)] = ck[span(k), :].T
        grad[...] += jnp.dot(ct[:, span(k)], x[span(k), :], preferred_element_type=F32)

    pair_copy(f_all, 0).wait()
    projected = jnp.dot(
        grad[...].astype(BF16), f_all[...].reshape(grad.shape[1], f_all.shape[-1]), preferred_element_type=F32
    )
    rank = projected.shape[1] // FS
    part[:, :, :width] = projected.T.reshape(FS, rank, width).astype(BF16)

    for peer in FARTHEST:

        @pl.when(me != peer)
        def _():
            remote(part.at[peer], parts.at[me], sum_sem.at[0], sum_sem.at[1], fs=peer).start()

    relay(w_all, 1, (1, 3, 2))
    for copy in small[2:]:
        copy.wait()
    seen = parts.at[pl.ds(0, FS - 1)]
    remote(seen, seen, sum_sem.at[0], sum_sem.at[1], fs=partner).wait()
    parts[me] = part[me]
    summed = parts[...].astype(F32).sum(axis=0)
    total[...] = summed
    for low, high, first, second in ((0, kv, mk, vk), (kv, width, mq, vq)):
        got = summed[:, low:high]
        first_new = 0.8 * first[...] + 0.2 * got
        second_new = 0.9 * second[...] + 0.1 * got * got
        direction = first_new / (jnp.sqrt(second_new) + 1e-08)
        d_all[me, :, low:high] = direction.astype(BF16)
    mine = d_all.at[me]

    for peer in NEAREST:

        @pl.when(me != peer)
        def _():
            remote(mine, mine, dir_sem.at[0], dir_sem.at[1], fs=peer).start()

    lane = lax.broadcasted_iota(jnp.int32, (1, 128), 1)

    def lengths(rows):
        columns = jnp.sum(rows * rows, axis=0, keepdims=True)
        return jnp.where(
            lane < 64,
            jnp.sum(columns[:, :kv], axis=1, keepdims=True),
            jnp.sum(columns[:, kv:width], axis=1, keepdims=True),
        )

    crossed[tp] = jnp.zeros_like(crossed[tp])
    own_square[...] = lengths(d_all[me].astype(F32))
    for d in (2, 1, 3):
        for peer in NEAREST:
            remote(
                own_square, crossed.at[tp, me], square_sem.at[0], square_sem.at[1], fs=peer, tp=(tp + d) % TP
            ).start()
    pair_start(w_all, 1)
    seen = d_all.at[pl.ds(0, FS - 1)]
    remote(seen, seen, dir_sem.at[0], dir_sem.at[1], fs=partner).wait()
    every = d_all[...].astype(F32).reshape(FS * rank, d_all.shape[-1])[:, :width]
    factor = f_all[...].reshape(l_steps.shape[0], f_all.shape[-1])
    directions = every.astype(BF16)
    own_steps[...] = jnp.dot(f_all[z, y, c], directions, preferred_element_type=F32)
    l_steps[...] = jnp.dot(factor, directions[:, :kv], preferred_element_type=F32)
    q_steps[...] = lax.dot_general(
        directions[:, kv:], factor, (((0,), (1,)), ((), ())), preferred_element_type=F32
    )
    plane_square = lengths(every)
    pair_copy(w_all, 1).wait()
    q_weights[...] = w_all[...].reshape(l_steps.shape[0], w_all.shape[-1])[:, kv:width].T
    seen = crossed.at[pl.ds(0, TP - 1)]
    remote(seen, seen, square_sem.at[0], square_sem.at[1], fs=partner, tp=tp).wait()
    squares[...] = plane_square + crossed[...].sum(axis=(0, 1))


def update_kernel(
    counts,
    w_all, q_weights, l_steps, q_steps, own_steps, squares, total, wq, wk, mq, mk, vq, vk,
    q_new, l_new, q_step, l_step, q_copy, l_copy, q_first, l_first, q_second, l_second,
):
    kv = wk.shape[1]
    width = kv + wq.shape[1]
    sums = squares[...]
    scales = [
        0.5 * jnp.sqrt(jnp.full((1, 1), counts[i], F32)) / jnp.sqrt(sums[:, 64 * i : 64 * i + 1] + 1e-06)
        for i in range(2)
    ]
    summed = total[...]
    for low, high, first, second, first_new, second_new in (
        (0, kv, mk, vk, l_first, l_second),
        (kv, width, mq, vq, q_first, q_second),
    ):
        got = summed[:, low:high]
        first_new[...] = 0.8 * first[...] + 0.2 * got
        second_new[...] = 0.9 * second[...] + 0.1 * got * got
    own = own_steps[...]
    for low, high, scale, weight, new, step in (
        (0, kv, scales[0], wk, l_new, l_step),
        (kv, width, scales[1], wq, q_new, q_step),
    ):
        taken = own[:, low:high] * scale
        step[...] = taken
        new[...] = weight[...] - taken
    weights = w_all[...].reshape(l_steps.shape[0], w_all.shape[-1])
    l_copy[...] = (weights[:, :kv].astype(F32) - l_steps[...] * scales[0]).astype(BF16)
    q_copy[...] = (q_weights[...].astype(F32) - q_steps[...] * scales[1]).astype(BF16)


def body(x, cq, ck, f, wq, wk, mq, mk, vq, vk):
    tokens, model = x.shape
    rows, rank = f.shape
    qw, kv = cq.shape[1], ck.shape[1]
    width = kv + qw
    lanes = -(-width // 128) * 128
    mine = rank // FS
    hbm = pl.BlockSpec(memory_space=pltpu.HBM)
    vmem = pl.BlockSpec(memory_space=pltpu.VMEM)
    shape = jax.ShapeDtypeStruct
    dma = pltpu.SemaphoreType.DMA
    gathered = pl.pallas_call(
        exchange_kernel,
        out_shape=(
            shape((Z, Y, CORES, rows, lanes), BF16),
            shape((qw, FS * rows), BF16),
            shape((FS * rows, kv), F32),
            shape((qw, FS * rows), F32),
            shape((rows, width), F32),
            shape((1, 128), F32),
            shape((mine, lanes), F32),
        ),
        in_specs=[hbm] * 10,
        out_specs=(vmem,) * 7,
        scratch_shapes=[
            pltpu.VMEM((Z, Y, CORES, rows, rank), BF16),
            pltpu.VMEM((FS, mine, lanes), BF16),
            pltpu.VMEM((tokens, model), BF16),
            pltpu.VMEM((tokens, kv), BF16),
            pltpu.VMEM((width, tokens), BF16),
            pltpu.VMEM((width, model), F32),
            pltpu.VMEM((rows, qw), F32),
            pltpu.VMEM((rows, kv), F32),
            pltpu.VMEM((mine, qw), F32),
            pltpu.VMEM((mine, kv), F32),
            pltpu.VMEM((mine, qw), F32),
            pltpu.VMEM((mine, kv), F32),
            pltpu.VMEM((FS, mine, lanes), BF16),
            pltpu.VMEM((FS, mine, lanes), BF16),
            pltpu.VMEM((TP, FS, 1, 128), F32),
            pltpu.VMEM((1, 128), F32),
            dma((tokens // CHUNK, 3)),
            dma((6,)),
            dma,
            dma((2, 2, 3)),
            dma((2, 2, 3)),
            dma((2, 2)),
            dma((2, 2)),
            dma((2, 2)),
            dma((2,)),
            dma((2,)),
            dma((2,)),
        ],
        compiler_params=pltpu.CompilerParams(
            collective_id=0, has_side_effects=True, vmem_limit_bytes=44 * 1024 * 1024
        ),
        name="exchange",
    )(*(pltpu.with_memory_space_constraint(a, pltpu.HBM) for a in (x, cq.T, ck, f, wq, wk, mq, mk, vq, vk)))
    counts = (rank * kv * TP, rank * qw * TP)
    model_rows = rows * FS
    like = lambda a: shape(a.shape, a.dtype)
    outs = pl.pallas_call(
        functools.partial(update_kernel, counts),
        out_shape=(
            like(wq), like(wk), like(wq), like(wk),
            shape((qw, model_rows), BF16), shape((model_rows, kv), BF16),
            like(mq), like(mk), like(vq), like(vk),
        ),
        in_specs=[vmem] * 13,
        out_specs=(vmem,) * 10,
        compiler_params=pltpu.CompilerParams(vmem_limit_bytes=16 * 1024 * 1024),
        name="update",
    )(*gathered, wq, wk, mq, mk, vq, vk)
    return outs[:4] + (outs[4].T,) + outs[5:]


def solution(mesh):
    return jax.shard_map(
        body,
        mesh=mesh,
        in_specs=(P("fs", None), P("fs", "tp"), P("fs", "tp"), P("fs", None)) + (P("fs", "tp"),) * 6,
        out_specs=(P("fs", "tp"),) * 4 + (P(None, "tp"),) * 2 + (P("fs", "tp"),) * 4,
        check_vma=False,
    )
```
